32 devices in a mesh: sp: 16 (over z, y, x), tp: 2 (over core).
Axes of the slice: x: 2, y: 2, z: 4, core: 2. Of those that a mesh axis runs over, the one named last changes fastest.
Arguments:
- stream: bfloat16 [4096, 2048], P('sp', 'tp'), may hold values from -6 to 6
- out_grad: bfloat16 [4096, 2048], P('sp', 'tp'), may hold values from -6 to 6
- gate_in: bfloat16 [4096, 1024], P('sp', 'tp'), may hold values from -6 to 6
- conv_gate: bfloat16 [4096, 1024], P('sp', 'tp'), may hold values from -6 to 6
- conv_value: bfloat16 [4096, 1024], P('sp', 'tp'), may hold values from -6 to 6
- taps: float32 [3, 1024], P(None, 'tp'), may hold values from -3.5 to 3.5
- w_out: bfloat16 [2048, 1024], P(None, 'tp'), may hold values from -0.1875 to 0.1875
- route_ids: int32 [4096, 2], P('sp'), may hold values from 0 to 15, all different within a row; in each aligned block of 256 rows (0 to 255, 256 to 511, ...) at most 64 rows name the same one
- route_weights: float32 [4096, 2], P('sp'), may hold values from 0.1 to 1
- w_gate: bfloat16 [16, 2048, 1024], P('sp', None, 'tp'), may hold values from -0.125 to 0.125
- w_up: bfloat16 [16, 2048, 1024], P('sp', None, 'tp'), may hold values from -0.125 to 0.125
- w_down: bfloat16 [16, 1024, 2048], P('sp', 'tp'), may hold values from -0.1875 to 0.1875
Outputs:
- stream_grad: bfloat16 [4096, 2048], P('sp', 'tp')
- gate_in_grad: bfloat16 [4096, 1024], P('sp', 'tp')
- conv_gate_grad: bfloat16 [4096, 1024], P('sp', 'tp')
- conv_value_grad: bfloat16 [4096, 1024], P('sp', 'tp')
- w_out_grad: float32 [2048, 1024], P('sp', 'tp')
- w_gate_grad: float32 [16, 2048, 1024], P('sp', None, 'tp')
- w_up_grad: float32 [16, 2048, 1024], P('sp', None, 'tp')
- w_down_grad: float32 [16, 1024, 2048], P('sp', 'tp')
The draws below stay inside these ranges and needn't reach their ends.
Inputs may be any that keep to these rules, and one draw needn't show every extreme that they name: `route_ids`: the ids of one token differ. Within each aligned block of 256 tokens (the rows of one index of sp), no expert is named by more than 64 routes, and in every draw some expert is named by exactly 64 routes of some block.
All inputs are finite; a program needn't handle non-finite values.
Results may differ from the reference program's by a relative error of at most 0.009.
Values may be sent and summed in bfloat16 or wider, within the bound.
No kernel may reach another device: no remote copies, remote signals or barrier semaphores. Data moves between devices by JAX's collectives and lax.ppermute only.
A program may use at most 128 MiB of HBM per device.

```python
import math
import jax
import jax.numpy as jnp
import numpy as np
from jax import lax

D = 2048
CW = 1024
FF = 1024
TOP = 2
TAPS = 3
EXPERTS = 16
TOK_DEV = 256
TOKENS = 4096
CAP = 64
EXPERT_ROWS = 1024
N_SP = 16
N_TP = 2


def strengthened(drawn, rng, source, target, parts, factor):
    owner, partner = [(jnp.arange(drawn.shape[position]) // (drawn.shape[position] // parts)).reshape([-1 if axis == position else 1 for axis in range(drawn.ndim)]) for position in (source, target)]
    chosen = jax.random.permutation(rng, parts)[partner]
    strong = (owner == chosen) | (owner == (partner + parts // 2) % parts)
    return jnp.where(strong, factor * drawn, drawn)


def level_of(own_key, dims, pieces, smallest, high):
    def one(position, blocks):
        steps = jax.random.uniform(jax.random.fold_in(jax.random.fold_in(own_key, 6), position), (blocks,), jnp.float32, smallest / len(pieces), high / len(pieces))
        return jnp.repeat(jnp.exp(steps), dims[position] // blocks).reshape((-1,) + (1,) * (len(dims) - position - 1))

    factor_of = one(*pieces[0])
    for cut in pieces[1:]:
        factor_of = factor_of * one(*cut)
    return factor_of


def deal_out(stream_key, own, number, rows, count, top, bound, lean):
    ranking = jax.random.permutation(stream_key, count)
    packed, usual = shares(count, rows * top, bound, lean, True), shares(count, rows * top, bound, lean, False)
    places = jnp.arange(count)

    def named(sizes, turn):
        used = int((sizes > 0).sum())
        fixed = max(1, used // 4)
        passed = fixed + (places - fixed + turn * (used - fixed)) % max(1, count - fixed)
        return jnp.zeros((count,), jnp.int32).at[ranking[jnp.where(places < fixed, places, passed)]].set(jnp.asarray(sizes, jnp.int32))

    sizes = jnp.where(number % 4 == 0, named(packed, number // 4), named(usual, number - number // 4 - 1))
    mixed = jax.random.permutation(jax.random.fold_in(own, 3), count)
    giver, taker = mixed[0:count // 2 * 2:2], mixed[1:count // 2 * 2:2]
    room = jnp.minimum(sizes[giver] - 1, bound - sizes[taker]) // 2
    room = jnp.where((giver == ranking[0]) | (taker == ranking[0]) | (sizes[taker] == 0), 0, jnp.maximum(room, 0))
    passed = jax.random.randint(jax.random.fold_in(own, 4), (count // 2,), 0, 1 << 20) % (room + 1)
    sizes = sizes.at[giver].add(-passed).at[taker].add(passed)
    items = jnp.searchsorted(jnp.cumsum(sizes), jnp.arange(rows * top), side="right").astype(jnp.int32)
    listing = items.reshape(top, rows).T
    listing = listing[jax.random.permutation(jax.random.fold_in(own, 1), rows)]
    turn = jax.random.randint(jax.random.fold_in(own, 2), (rows, 1), 0, top)
    return jnp.take_along_axis(listing, (jnp.arange(top)[None, :] + turn) % top, axis=1)


def shares(amount, total, most, skew, full):
    loads = [(1 << 20) // math.isqrt(grade ** skew) + 1 for grade in range(1, amount + 1)]
    largest = most if full else min(most, max(-(-total // amount), total * loads[0] // sum(loads)))
    least = 1 if total - largest >= amount - 1 else 0
    given, rest = [largest] + [least] * (amount - 1), total - largest - least * (amount - 1)
    while rest > 0:
        free = [i for i in range(1, amount) if given[i] < largest] or [i for i in range(1, amount) if given[i] < most]
        whole, left = sum([loads[i] for i in free]), rest
        for i in free:
            addition = min(most - given[i], max(1, left * loads[i] // whole), rest)
            given[i] = given[i] + addition
            rest = rest - addition
    return np.array(given)


def scatter_about(own_key, dims, scale, limit, split=(), kind=jnp.bfloat16):
    array = scale * jax.random.normal(own_key, dims, jnp.float32)
    if split:
        array = array * level_of(own_key, dims, split, -0.22, 0.18)
    return jnp.clip(array, -limit, limit).astype(kind)


def gaussian_with(rng, extent, width, most, pieces, heavy, held_as=jnp.bfloat16):
    result = width * jax.random.normal(rng, extent, jnp.float32)
    if pieces:
        result = result * level_of(rng, extent, pieces, -0.22, 0.18)
    return jnp.clip(strengthened(result, jax.random.fold_in(rng, 3), *heavy), -most, most).astype(held_as)


def setup_inputs(seed: int = 0) -> dict:
    key_list = jax.random.split(jax.random.key(seed), 13)
    stream = scatter_about(key_list[0], (TOKENS, D), 1.0, 6.0, ((0, 16), (1, 2)))
    out_grad = gaussian_with(key_list[1], (TOKENS, D), 1.0, 6.0, ((0, 16), (1, 2)), (0, 1, 16, 2.0))
    gate_in = scatter_about(key_list[2], (TOKENS, CW), 1.0, 6.0, ((0, 16), (1, 2)))
    conv_gate = scatter_about(key_list[3], (TOKENS, CW), 1.0, 6.0, ((0, 16), (1, 2)))
    conv_value = scatter_about(key_list[4], (TOKENS, CW), 1.0, 6.0, ((0, 16), (1, 2)))
    taps = scatter_about(key_list[5], (TAPS, CW), TAPS ** -0.5, 3.5, ((1, 2),), jnp.float32)
    w_out = scatter_about(key_list[6], (D, CW), CW ** -0.5, 0.1875, ((1, 2),))
    route_ids_keys = jax.random.split(jax.random.fold_in(key_list[7], 1), TOKENS // TOK_DEV)
    route_ids_turns = jax.random.permutation(jax.random.fold_in(key_list[7], 3), TOKENS // TOK_DEV)
    route_ids = jax.vmap(lambda own, number: deal_out(jax.random.fold_in(key_list[7], 2), own, number, TOK_DEV, EXPERTS, TOP, CAP, 2))(route_ids_keys, route_ids_turns).reshape((TOKENS, TOP))
    route_weights = jnp.clip(0.1 + 0.9 * jax.random.uniform(key_list[8], (TOKENS, TOP), jnp.float32) ** level_of(key_list[8], (TOKENS, TOP), ((0, 16),), -0.2, 0.2), 0.1, 1.0)
    w_gate = scatter_about(key_list[9], (EXPERTS, D, FF), D ** -0.5, 0.125, ((0, 16), (2, 2)))
    w_up = scatter_about(key_list[10], (EXPERTS, D, FF), D ** -0.5, 0.125, ((0, 16), (2, 2)))
    w_down = scatter_about(key_list[11], (EXPERTS, FF, D), FF ** -0.5, 0.1875, ((0, 16), (1, 2)))
    return {"stream": stream, "out_grad": out_grad, "gate_in": gate_in, "conv_gate": conv_gate, "conv_value": conv_value, "taps": taps, "w_out": w_out, "route_ids": route_ids, "route_weights": route_weights, "w_gate": w_gate, "w_up": w_up, "w_down": w_down}


def expert_step(carry_rows, stream_pad, cot_pad):
    table_row, gate_weight, up_weight, down_weight = carry_rows
    routes_total = TOKENS * TOP
    token_index = jnp.where(table_row < routes_total, table_row // TOP, TOKENS).astype(jnp.int32)
    expert_in = stream_pad[token_index]
    expert_cot = cot_pad[table_row]
    pre_gate = jnp.dot(expert_in, gate_weight, preferred_element_type=jnp.float32)
    pre_up = jnp.dot(expert_in, up_weight, preferred_element_type=jnp.float32)
    sigmoid_gate = jax.nn.sigmoid(pre_gate)
    silu_gate = pre_gate * sigmoid_gate
    hidden = (silu_gate * pre_up).astype(jnp.bfloat16)
    hidden_grad = jnp.dot(expert_cot, down_weight.T, preferred_element_type=jnp.float32)
    down_grad = jnp.dot(hidden.T, expert_cot, preferred_element_type=jnp.float32)
    up_grad = (hidden_grad * silu_gate).astype(jnp.bfloat16)
    gate_grad = (hidden_grad * pre_up * sigmoid_gate * (1.0 + pre_gate * (1.0 - sigmoid_gate))).astype(jnp.bfloat16)
    gate_w_grad = jnp.dot(expert_in.T, gate_grad, preferred_element_type=jnp.float32)
    up_w_grad = jnp.dot(expert_in.T, up_grad, preferred_element_type=jnp.float32)
    block_width = FF // N_TP
    running = jnp.zeros((EXPERT_ROWS, D), jnp.float32)
    for block_index in range(N_TP):
        lower = block_index * block_width
        upper = lower + block_width
        partial_term = jnp.dot(gate_grad[:, lower:upper], gate_weight[:, lower:upper].T, preferred_element_type=jnp.float32)
        partial_term = partial_term + jnp.dot(up_grad[:, lower:upper], up_weight[:, lower:upper].T, preferred_element_type=jnp.float32)
        rounded = lax.optimization_barrier(partial_term.astype(jnp.bfloat16))
        running = running + rounded.astype(jnp.float32)
    return gate_w_grad, up_w_grad, down_grad, running.astype(jnp.bfloat16)


def reference(stream, out_grad, gate_in, conv_gate, conv_value, taps, w_out, route_ids, route_weights, w_gate, w_up, w_down):
    prod_rows = conv_gate.astype(jnp.float32) * conv_value.astype(jnp.float32)
    padded = jnp.concatenate([jnp.zeros((TAPS - 1, CW), jnp.float32), prod_rows], axis=0)
    conv_sum = jnp.zeros((TOKENS, CW), jnp.float32)
    for tap_index in range(TAPS):
        conv_sum = conv_sum + taps[tap_index][None, :] * padded[tap_index:tap_index + TOKENS]
    mixer_out = (gate_in.astype(jnp.float32) * conv_sum).astype(jnp.bfloat16)

    routes_dev = TOK_DEV * TOP
    route_block = route_ids.reshape(N_SP, routes_dev)
    one_hot = (route_block[:, :, None] == jnp.arange(EXPERTS, dtype=jnp.int32)[None, None, :]).astype(jnp.int32)
    slot_pos = jnp.sum(jnp.cumsum(one_hot, axis=1) * one_hot, axis=2) - 1
    source_index = jnp.arange(N_SP, dtype=jnp.int32)[:, None]
    flat_slot = (route_block * EXPERT_ROWS + source_index * CAP + slot_pos).reshape(-1).astype(jnp.int32)
    routes_total = TOKENS * TOP
    table = jnp.full((EXPERTS * EXPERT_ROWS,), routes_total, jnp.int32)
    table = table.at[flat_slot].set(jnp.arange(routes_total, dtype=jnp.int32))
    table = table.reshape(EXPERTS, EXPERT_ROWS)

    stream_pad = jnp.concatenate([stream, jnp.zeros((1, D), jnp.bfloat16)], axis=0)
    scaled = (route_weights[:, :, None] * out_grad[:, None, :].astype(jnp.float32)).astype(jnp.bfloat16)
    cot_pad = jnp.concatenate([scaled.reshape(routes_total, D), jnp.zeros((1, D), jnp.bfloat16)], axis=0)

    def per_expert(carry_rows):
        return expert_step(carry_rows, stream_pad, cot_pad)

    w_gate_grad, w_up_grad, w_down_grad, row_grad = lax.map(per_expert, (table, w_gate, w_up, w_down))
    row_flat = row_grad.reshape(EXPERTS * EXPERT_ROWS, D)
    route_rows = row_flat[flat_slot].astype(jnp.float32).reshape(TOKENS, TOP, D)
    input_grad = jnp.sum(route_rows, axis=1)
    stream_grad = (out_grad.astype(jnp.float32) + input_grad).astype(jnp.bfloat16)

    w_out_grad = jnp.dot(stream_grad.T, mixer_out, preferred_element_type=jnp.float32)
    mixer_grad = jnp.dot(stream_grad, w_out, preferred_element_type=jnp.float32).astype(jnp.bfloat16)
    gate_in_grad = (mixer_grad.astype(jnp.float32) * conv_sum).astype(jnp.bfloat16)
    conv_inner = mixer_grad.astype(jnp.float32) * gate_in.astype(jnp.float32)
    padded_back = jnp.concatenate([conv_inner, jnp.zeros((TAPS - 1, CW), jnp.float32)], axis=0)
    prod_grad = jnp.zeros((TOKENS, CW), jnp.float32)
    for tap_index in range(TAPS):
        offset = TAPS - 1 - tap_index
        prod_grad = prod_grad + taps[tap_index][None, :] * padded_back[offset:offset + TOKENS]
    conv_gate_grad = (prod_grad * conv_value.astype(jnp.float32)).astype(jnp.bfloat16)
    conv_value_grad = (prod_grad * conv_gate.astype(jnp.float32)).astype(jnp.bfloat16)
    return (stream_grad, gate_in_grad, conv_gate_grad, conv_value_grad, w_out_grad, w_gate_grad, w_up_grad, w_down_grad)
```

```python
import jax
import jax.numpy as jnp
from jax import lax
from jax.sharding import PartitionSpec as P

BF = jnp.bfloat16
F32 = jnp.float32


def passed_along(shard, axis, by):
    count = lax.axis_size(axis)
    pairs = [(i, i + by) for i in range(count) if 0 <= i + by < count]
    return lax.ppermute(shard, axis, pairs)


def swapped(shard):
    return lax.ppermute(shard, "tp", [(0, 1), (1, 0)])


def exchanged(blocks, groups=None):
    return lax.all_to_all(
        blocks, "sp", split_axis=0, concat_axis=0, tiled=True, axis_index_groups=groups
    )


def in_order(mine, other, first, axis):
    return jnp.where(
        first,
        jnp.concatenate([mine, other], axis=axis),
        jnp.concatenate([other, mine], axis=axis),
    )


def mm(left, right, dims):
    return lax.dot_general(left, right, (dims, ((), ())), preferred_element_type=F32)


def shards(
    stream,
    out_grad,
    gate_in,
    conv_gate,
    conv_value,
    taps,
    w_out,
    route_ids,
    route_weights,
    w_gate,
    w_up,
    w_down,
):
    tok_rows, half_width = stream.shape
    width = 2 * half_width
    sp_count = lax.axis_size("sp")
    experts = w_gate.shape[0] * sp_count
    capacity = 4 * tok_rows // experts
    part = capacity // 2
    slots = experts * part
    tp = lax.axis_index("tp")
    first = tp == 0

    stream_full = in_order(stream, swapped(stream), first, 1)
    out_full = in_order(out_grad, swapped(out_grad), first, 1)

    ids = route_ids.T
    expert_of = jnp.arange(experts, dtype=jnp.int32)
    hit = ids[:, None, :] == expert_of[None, :, None]
    named = jnp.any(hit, axis=0)
    weight_of = jnp.sum(jnp.where(hit, route_weights.T[:, None, :], 0.0), axis=0)
    before = jnp.arange(tok_rows)[:, None] < jnp.arange(tok_rows)[None, :]
    rank = mm(named.astype(BF), before.astype(BF), ((1,), (0,)))
    slot_of = jnp.where(named, rank.astype(jnp.int32) - tp * part, -1)
    chosen = slot_of[:, None, :] == jnp.arange(part, dtype=jnp.int32)[None, :, None]
    pick = chosen.astype(BF).reshape(slots, tok_rows)
    slot_weight = jnp.sum(jnp.where(chosen, weight_of[:, None, :], 0.0), axis=2).reshape(slots, 1)

    send_rows = mm(pick, stream_full, ((1,), (0,))).astype(BF)
    send_cot = (mm(pick, out_full, ((1,), (0,))) * slot_weight).astype(BF)
    rows = exchanged(send_rows.reshape(experts, part, width)).reshape(slots, width)
    cot = exchanged(send_cot.reshape(experts, part, width)).reshape(slots, width)

    gate_all = jnp.concatenate([w_gate[0], swapped(w_gate[0])], axis=1)
    up_all = jnp.concatenate([w_up[0], swapped(w_up[0])], axis=1)
    down_all = jnp.concatenate([w_down[0], swapped(w_down[0])], axis=0)
    hid = w_gate.shape[2]

    pre_gate = mm(rows, gate_all, ((1,), (0,)))
    pre_up = mm(rows, up_all, ((1,), (0,)))
    sigmoid_gate = jax.nn.sigmoid(pre_gate)
    silu_gate = pre_gate * sigmoid_gate
    hidden = (silu_gate * pre_up).astype(BF)
    slope = pre_up * sigmoid_gate * (1.0 + pre_gate * (1.0 - sigmoid_gate))
    hidden_grad = mm(cot, down_all, ((1,), (1,)))
    up_grad = (hidden_grad * silu_gate).astype(BF)
    gate_grad = (hidden_grad * slope).astype(BF)
    row_grad = mm(gate_grad, gate_all, ((1,), (1,))) + mm(up_grad, up_all, ((1,), (1,)))
    back = exchanged(row_grad.astype(BF).reshape(experts, part, width)).reshape(slots, width)

    rows_other = swapped(rows)
    cot_other = swapped(cot)
    gate_other = swapped(gate_grad[:, hid:])
    up_other = swapped(up_grad[:, hid:])
    hidden_other = swapped(hidden[:, hid:])
    gate_w_grad = mm(rows, gate_grad[:, :hid], ((0,), (0,))) + mm(rows_other, gate_other, ((0,), (0,)))
    up_w_grad = mm(rows, up_grad[:, :hid], ((0,), (0,))) + mm(rows_other, up_other, ((0,), (0,)))
    down_w_grad = mm(hidden[:, :hid], cot, ((0,), (0,))) + mm(hidden_other, cot_other, ((0,), (0,)))

    mine = mm(pick, back, ((0,), (0,))).astype(BF)
    stream_whole = (
        out_full.astype(F32) + (mine.astype(F32) + swapped(mine).astype(F32))
    ).astype(BF)
    stream_half = jnp.where(first, stream_whole[:, :half_width], stream_whole[:, half_width:])

    depth = taps.shape[0]
    channels = conv_gate.shape[1]
    prod_rows = conv_gate.astype(F32) * conv_value.astype(F32)
    left_rows = passed_along(prod_rows[tok_rows - depth + 1 :], "sp", 1)
    padded = jnp.concatenate([left_rows, prod_rows], axis=0)
    conv_sum = jnp.zeros((tok_rows, channels), F32)
    for tap_index in range(depth):
        conv_sum = conv_sum + taps[tap_index][None, :] * padded[tap_index : tap_index + tok_rows]
    mixer_out = (gate_in.astype(F32) * conv_sum).astype(BF)

    mixer_grad = mm(stream_whole, w_out, ((1,), (0,))).astype(BF)
    mixer_wide = mixer_grad.astype(F32)
    gate_in_grad = (mixer_wide * conv_sum).astype(BF)
    conv_inner = mixer_wide * gate_in.astype(F32)
    right_rows = passed_along(conv_inner[: depth - 1], "sp", -1)
    padded_back = jnp.concatenate([conv_inner, right_rows], axis=0)
    prod_grad = jnp.zeros((tok_rows, channels), F32)
    for tap_index in range(depth):
        offset = depth - 1 - tap_index
        prod_grad = prod_grad + taps[tap_index][None, :] * padded_back[offset : offset + tok_rows]
    conv_gate_grad = (prod_grad * conv_value.astype(F32)).astype(BF)
    conv_value_grad = (prod_grad * conv_gate.astype(F32)).astype(BF)

    inner_count = 1 << ((sp_count.bit_length() - 1) // 2)
    outer_count = sp_count // inner_count
    inner_groups = [[o * inner_count + i for i in range(inner_count)] for o in range(outer_count)]
    outer_groups = [[o * inner_count + i for o in range(outer_count)] for i in range(inner_count)]
    wide_mixer = exchanged(
        jnp.broadcast_to(mixer_out[None], (inner_count, tok_rows, channels)), inner_groups
    ).reshape(inner_count * tok_rows, channels)
    block = width // sp_count
    half_outer = outer_count // 2
    by_inner = stream_half.reshape(tok_rows, half_outer, inner_count, block)
    by_inner = jnp.transpose(by_inner, (2, 0, 1, 3)).reshape(inner_count, tok_rows, half_outer * block)
    features = exchanged(by_inner, inner_groups).reshape(inner_count * tok_rows, half_outer * block)
    features = in_order(features, swapped(features), first, 1)
    partial = mm(features, wide_mixer, ((0,), (0,))).astype(BF)
    parts = exchanged(partial.reshape(outer_count, block, channels), outer_groups)
    out_proj_grad = jnp.sum(parts.astype(F32), axis=0)

    return (
        stream_half,
        gate_in_grad,
        conv_gate_grad,
        conv_value_grad,
        out_proj_grad,
        gate_w_grad[None],
        up_w_grad[None],
        down_w_grad[None],
    )


def solution(mesh):
    placed = (
        P("sp", "tp"),
        P("sp", "tp"),
        P("sp", "tp"),
        P("sp", "tp"),
        P("sp", "tp"),
        P(None, "tp"),
        P(None, "tp"),
        P("sp", None),
        P("sp", None),
        P("sp", None, "tp"),
        P("sp", None, "tp"),
        P("sp", "tp", None),
    )
    return jax.shard_map(
        shards,
        mesh=mesh,
        in_specs=placed,
        out_specs=(
            P("sp", "tp"),
            P("sp", "tp"),
            P("sp", "tp"),
            P("sp", "tp"),
            P("sp", "tp"),
            P("sp", None, "tp"),
            P("sp", None, "tp"),
            P("sp", "tp", None),
        ),
        check_vma=False,
    )
```

```python
import jax
import jax.numpy as jnp
from jax import lax
from jax.sharding import PartitionSpec as P

BF = jnp.bfloat16
F32 = jnp.float32


def passed_along(shard, axis, by):
    count = lax.axis_size(axis)
    pairs = [(i, i + by) for i in range(count) if 0 <= i + by < count]
    return lax.ppermute(shard, axis, pairs)


def swapped(shard):
    return lax.ppermute(shard, "tp", [(0, 1), (1, 0)])


def exchanged(blocks, groups=None):
    return lax.all_to_all(
        blocks, "sp", split_axis=0, concat_axis=0, tiled=True, axis_index_groups=groups
    )


def in_order(mine, other, first, axis):
    return jnp.where(
        first,
        jnp.concatenate([mine, other], axis=axis),
        jnp.concatenate([other, mine], axis=axis),
    )


def mm(left, right, dims):
    return lax.dot_general(left, right, (dims, ((), ())), preferred_element_type=F32)


def shards(
    stream,
    out_grad,
    gate_in,
    conv_gate,
    conv_value,
    taps,
    w_out,
    route_ids,
    route_weights,
    w_gate,
    w_up,
    w_down,
):
    tok_rows, half_width = stream.shape
    width = 2 * half_width
    sp_count = lax.axis_size("sp")
    experts = w_gate.shape[0] * sp_count
    capacity = 4 * tok_rows // experts
    part = capacity // 2
    slots = experts * part
    tp = lax.axis_index("tp")
    first = tp == 0

    half = sp_count // 2
    half_experts = experts // 2
    upper = lax.axis_index("sp") >= half

    def traded(shard):
        return lax.ppermute(shard, "sp", [(i, i ^ half) for i in range(sp_count)])

    facts = jnp.concatenate([route_ids.T.astype(F32), route_weights.T], axis=0)
    facts = jnp.concatenate([facts, traded(facts)], axis=1)
    stream_there = traded(stream)
    out_there = traded(out_grad)
    stream_full = in_order(stream, swapped(stream), first, 1)
    out_full = in_order(out_grad, swapped(out_grad), first, 1)
    stream_pair = jnp.concatenate(
        [stream_full, in_order(stream_there, swapped(stream_there), first, 1)], axis=0
    )
    out_pair = jnp.concatenate([out_full, in_order(out_there, swapped(out_there), first, 1)], axis=0)

    top_count = route_ids.shape[1]
    pair_ids, pair_weights = facts[:top_count].astype(jnp.int32), facts[top_count:]
    place = jnp.arange(2 * tok_rows, dtype=jnp.int32)
    block_of = place // tok_rows
    half_of = jnp.where(upper, 1 - block_of, block_of)

    def ranks(ids, expert_of, blocks):
        hit = ids[:, None, :] == expert_of[None, :, None]
        named = jnp.any(hit, axis=0)
        at = place[: blocks.shape[0]]
        before = (at[:, None] < at[None, :]) & (blocks[:, None] == blocks[None, :])
        rank = mm(named.astype(BF), before.astype(BF), ((1,), (0,)))
        return hit, jnp.where(named, rank.astype(jnp.int32) - tp * part, -1)

    slot_at = jnp.arange(part, dtype=jnp.int32)
    _, slot_home = ranks(route_ids.T, jnp.arange(experts, dtype=jnp.int32), block_of[:tok_rows])
    pick_home = (slot_home[:, None, :] == slot_at[None, :, None]).astype(BF).reshape(slots, tok_rows)
    here = jnp.arange(half_experts, dtype=jnp.int32) + jnp.where(upper, half_experts, 0)
    hit, slot_of = ranks(pair_ids, here, block_of)
    weight_of = jnp.sum(jnp.where(hit, pair_weights[:, None, :], 0.0), axis=0)
    chosen = (slot_of[:, None, None, :] == slot_at[None, None, :, None]) & (
        half_of[None, None, None, :] == jnp.arange(2, dtype=jnp.int32)[None, :, None, None]
    )
    pick = chosen.astype(BF).reshape(slots, 2 * tok_rows)
    slot_weight = jnp.sum(jnp.where(chosen, weight_of[:, None, None, :], 0.0), axis=3).reshape(slots, 1)

    half_groups = [[h * half + i for i in range(half)] for h in range(2)]
    send_rows = mm(pick, stream_pair, ((1,), (0,))).astype(BF)
    send_cot = (mm(pick, out_pair, ((1,), (0,))) * slot_weight).astype(BF)
    rows = exchanged(send_rows.reshape(half, 2 * part, width), half_groups).reshape(slots, width)
    cot = exchanged(send_cot.reshape(half, 2 * part, width), half_groups).reshape(slots, width)

    gate_all = jnp.concatenate([w_gate[0], swapped(w_gate[0])], axis=1)
    up_all = jnp.concatenate([w_up[0], swapped(w_up[0])], axis=1)
    down_all = jnp.concatenate([w_down[0], swapped(w_down[0])], axis=0)
    hid = w_gate.shape[2]

    pre_gate = mm(rows, gate_all, ((1,), (0,)))
    pre_up = mm(rows, up_all, ((1,), (0,)))
    sigmoid_gate = jax.nn.sigmoid(pre_gate)
    silu_gate = pre_gate * sigmoid_gate
    hidden = (silu_gate * pre_up).astype(BF)
    slope = pre_up * sigmoid_gate * (1.0 + pre_gate * (1.0 - sigmoid_gate))
    hidden, silu_gate, slope = lax.optimization_barrier((hidden, silu_gate, slope))
    both_all = jnp.concatenate([gate_all, up_all], axis=1)
    hidden_grad = mm(cot, down_all, ((1,), (1,)))
    up_grad = (hidden_grad * silu_gate).astype(BF)
    gate_grad = (hidden_grad * slope).astype(BF)
    both_grad = jnp.concatenate([gate_grad, up_grad], axis=1)
    row_grad = mm(both_grad, both_all, ((1,), (1,))).astype(BF)
    row_grad = jnp.transpose(row_grad.reshape(half, 2, part, width), (1, 0, 2, 3))
    back = exchanged(row_grad.reshape(experts, part, width)).reshape(slots, width)

    rows_both = jnp.concatenate([rows, swapped(rows)], axis=0)
    cot_both = jnp.concatenate([cot, swapped(cot)], axis=0)
    gate_both = jnp.concatenate([gate_grad[:, :hid], swapped(gate_grad[:, hid:])], axis=0)
    up_both = jnp.concatenate([up_grad[:, :hid], swapped(up_grad[:, hid:])], axis=0)
    hidden_both = jnp.concatenate([hidden[:, :hid], swapped(hidden[:, hid:])], axis=0)
    gate_w_grad = mm(rows_both, gate_both, ((0,), (0,)))
    up_w_grad = mm(rows_both, up_both, ((0,), (0,)))
    down_w_grad = mm(hidden_both, cot_both, ((0,), (0,)))

    mine = mm(pick_home, back, ((0,), (0,))).astype(BF)
    stream_whole = (
        out_full.astype(F32) + (mine.astype(F32) + swapped(mine).astype(F32))
    ).astype(BF)
    stream_half = jnp.where(first, stream_whole[:, :half_width], stream_whole[:, half_width:])

    depth = taps.shape[0]
    channels = conv_gate.shape[1]
    prod_rows = conv_gate.astype(F32) * conv_value.astype(F32)
    left_rows = passed_along(prod_rows[tok_rows - depth + 1 :], "sp", 1)
    padded = jnp.concatenate([left_rows, prod_rows], axis=0)
    conv_sum = jnp.zeros((tok_rows, channels), F32)
    for tap_index in range(depth):
        conv_sum = conv_sum + taps[tap_index][None, :] * padded[tap_index : tap_index + tok_rows]
    mixer_out = (gate_in.astype(F32) * conv_sum).astype(BF)

    mixer_grad = mm(stream_whole, w_out, ((1,), (0,))).astype(BF)
    mixer_wide = mixer_grad.astype(F32)
    gate_in_grad = (mixer_wide * conv_sum).astype(BF)
    conv_inner = mixer_wide * gate_in.astype(F32)
    right_rows = passed_along(conv_inner[: depth - 1], "sp", -1)
    padded_back = jnp.concatenate([conv_inner, right_rows], axis=0)
    prod_grad = jnp.zeros((tok_rows, channels), F32)
    for tap_index in range(depth):
        offset = depth - 1 - tap_index
        prod_grad = prod_grad + taps[tap_index][None, :] * padded_back[offset : offset + tok_rows]
    conv_gate_grad = (prod_grad * conv_value.astype(F32)).astype(BF)
    conv_value_grad = (prod_grad * conv_gate.astype(F32)).astype(BF)

    inner_count = 1 << ((sp_count.bit_length() - 1) // 2)
    outer_count = sp_count // inner_count
    inner = lax.rem(lax.axis_index("sp"), inner_count)

    def across(shard, step):
        return lax.ppermute(shard, "sp", [(i, i ^ step) for i in range(sp_count)])

    wide_mixer = jnp.concatenate([mixer_out] + [across(mixer_out, step) for step in range(1, inner_count)], axis=0)
    block = width // sp_count
    half_outer = outer_count // 2
    pieces = []
    for step in range(inner_count):
        piece = jnp.concatenate(
            [
                lax.dynamic_slice_in_dim(
                    stream_half, (o * inner_count + (inner ^ step)) * block, block, 1
                )
                for o in range(half_outer)
            ],
            axis=1,
        )
        pieces.append(across(piece, step) if step else piece)
    features = jnp.concatenate(pieces, axis=0)
    features = in_order(features, swapped(features), first, 1)
    partial = mm(features, wide_mixer, ((0,), (0,))).astype(BF).reshape(outer_count, block, channels)
    outer = lax.div(lax.axis_index("sp"), inner_count)
    out_proj_grad = lax.dynamic_index_in_dim(partial, outer, 0, keepdims=False).astype(F32)
    for step in range(outer_count - 1, 0, -1):
        piece = lax.dynamic_index_in_dim(partial, outer ^ step, 0, keepdims=False)
        piece = across(piece, step * inner_count)
        out_proj_grad = out_proj_grad + piece.astype(F32)

    return (
        stream_half,
        gate_in_grad,
        conv_gate_grad,
        conv_value_grad,
        out_proj_grad,
        gate_w_grad[None],
        up_w_grad[None],
        down_w_grad[None],
    )


def solution(mesh):
    placed = (
        P("sp", "tp"),
        P("sp", "tp"),
        P("sp", "tp"),
        P("sp", "tp"),
        P("sp", "tp"),
        P(None, "tp"),
        P(None, "tp"),
        P("sp", None),
        P("sp", None),
        P("sp", None, "tp"),
        P("sp", None, "tp"),
        P("sp", "tp", None),
    )
    return jax.shard_map(
        shards,
        mesh=mesh,
        in_specs=placed,
        out_specs=(
            P("sp", "tp"),
            P("sp", "tp"),
            P("sp", "tp"),
            P("sp", "tp"),
            P("sp", "tp"),
            P("sp", None, "tp"),
            P("sp", None, "tp"),
            P("sp", "tp", None),
        ),
        check_vma=False,
    )
```

```python
import functools
import jax
import jax.numpy as jnp
from jax import lax
from jax.experimental import pallas as pl
from jax.experimental.pallas import tpu as pltpu
from jax.sharding import PartitionSpec as P

BF = jnp.bfloat16
F32 = jnp.float32


def passed_along(shard, axis, by):
    count = lax.axis_size(axis)
    pairs = [(i, i + by) for i in range(count) if 0 <= i + by < count]
    return lax.ppermute(shard, axis, pairs)


def swapped(shard):
    return lax.ppermute(shard, "tp", [(0, 1), (1, 0)])


def exchanged(blocks, groups=None):
    return lax.all_to_all(
        blocks, "sp", split_axis=0, concat_axis=0, tiled=True, axis_index_groups=groups
    )


def in_order(mine, other, first, axis):
    return jnp.where(
        first,
        jnp.concatenate([mine, other], axis=axis),
        jnp.concatenate([other, mine], axis=axis),
    )


def mm(left, right, dims):
    return lax.dot_general(left, right, (dims, ((), ())), preferred_element_type=F32)


def back_kernel(first_steps, half_outer, inner_count, part, cot, down, silu, slope, gate, up, gate_grad, up_grad, row_grad):
    step = pl.program_id(0)
    tile = silu.shape[1]

    @pl.when(step < first_steps)
    def _():
        hidden_grad = mm(cot[...], down[...], ((1,), (1,)))
        at = pl.ds(pl.multiple_of(step * tile, tile), tile)
        gate_grad[:, at] = (hidden_grad * slope[...]).astype(BF)
        up_grad[:, at] = (hidden_grad * silu[...]).astype(BF)

    @pl.when(step >= first_steps)
    def _():
        cut, units = gate.shape[0] * gate.shape[2], gate.shape[3]
        rows = mm(gate_grad[...], gate[...].reshape(cut, units), ((1,), (1,)))
        rows += mm(up_grad[...], up[...].reshape(cut, units), ((1,), (1,)))
        for h in range(2):
            for o in range(half_outer):
                picked = []
                for i in range(inner_count):
                    at = ((o * inner_count + i) * 2 + h) * part
                    picked.append(rows[at : at + part])
                row_grad[h * half_outer + o, 0] = jnp.concatenate(picked, axis=0).astype(BF)


def row_grads(cot, down, silu, slope, gate, up, outer_count, inner_count, part):
    slots, width = cot.shape
    units = down.shape[0]
    tile, cut = min(units, 512), width // inner_count
    block = cut // outer_count
    first_steps = units // tile

    def early(i):
        return jnp.minimum(i, first_steps - 1)

    def late(i):
        return jnp.maximum(i - first_steps, 0)

    by_group = (outer_count, inner_count, block, units)
    kept = pl.BlockSpec((slots, units), lambda i: (0, 0))
    cols = pl.BlockSpec((slots, tile), lambda i: (0, early(i)))
    group = pl.BlockSpec((outer_count, 1, block, units), lambda i: (0, late(i), 0, 0))
    return pl.pallas_call(
        functools.partial(back_kernel, first_steps, outer_count // 2, inner_count, part),
        grid=(first_steps + inner_count,),
        in_specs=[
            pl.BlockSpec((slots, width), lambda i: (0, 0)),
            pl.BlockSpec((tile, width), lambda i: (early(i), 0)),
            cols,
            cols,
            group,
            group,
        ],
        out_specs=[
            kept,
            kept,
            pl.BlockSpec((outer_count, 1, inner_count * part, cut), lambda i: (0, late(i), 0, 0)),
        ],
        out_shape=[
            jax.ShapeDtypeStruct((slots, units), BF),
            jax.ShapeDtypeStruct((slots, units), BF),
            jax.ShapeDtypeStruct((outer_count, inner_count, inner_count * part, cut), BF),
        ],
        compiler_params=pltpu.CompilerParams(vmem_limit_bytes=62 * 2**20),
        cost_estimate=pl.CostEstimate(
            flops=6 * slots * width * units, bytes_accessed=8 * width * units, transcendentals=0
        ),
        name="row_grads",
    )(cot, down, silu, slope, gate.reshape(by_group), up.reshape(by_group))


def home_kernel(inner, pick, back, mine):
    tok_rows = pick.shape[0] // back.shape[1]
    experts, inner_count, part, cut = back.shape
    for j in range(inner_count):
        rows = back[:, inner[0] ^ j].astype(F32).reshape(experts * part, cut).astype(BF)
        at = slice(j * tok_rows, (j + 1) * tok_rows)
        mine[at] = mm(pick[at], rows, ((1,), (0,))).astype(BF)


def add_kernel(core, out_cut, mine, other, stream_cut, own_half):
    total = out_cut[...].astype(F32) + (mine[...].astype(F32) + other[...].astype(F32))
    total = total.astype(BF)
    stream_cut[...] = total
    wide = own_half.shape[1]
    own_half[...] = jnp.where(core[0] == 0, total[:, :wide], total[:, wide:])


def place_kernel(inner, block, *refs):
    pieces, out = refs[:-1], refs[-1]
    count = len(pieces)
    for j, piece in enumerate(pieces):
        for o in range(piece.shape[1] // block):
            at = pl.multiple_of((o * count + (inner[0] ^ j)) * block, block)
            out[:, pl.ds(at, block)] = piece[:, o * block : (o + 1) * block]


def local_kernel(kernel, shapes, scalar, *arrays):
    vmem = pl.BlockSpec(memory_space=pltpu.MemorySpace.VMEM)
    return pl.pallas_call(
        kernel,
        in_specs=[pl.BlockSpec(memory_space=pltpu.MemorySpace.SMEM)] + [vmem] * len(arrays),
        out_specs=[vmem] * len(shapes),
        out_shape=[jax.ShapeDtypeStruct(shape, BF) for shape in shapes],
        compiler_params=pltpu.CompilerParams(vmem_limit_bytes=24 * 2**20),
    )(scalar.astype(jnp.int32).reshape(1), *arrays)


def shards(
    stream,
    out_grad,
    gate_in,
    conv_gate,
    conv_value,
    taps,
    w_out,
    route_ids,
    route_weights,
    w_gate,
    w_up,
    w_down,
):
    tok_rows, half_width = stream.shape
    width = 2 * half_width
    sp_count = lax.axis_size("sp")
    experts = w_gate.shape[0] * sp_count
    capacity = 4 * tok_rows // experts
    part = capacity // 2
    slots = experts * part
    tp = lax.axis_index("tp")
    first = tp == 0

    inner_count = 1 << ((sp_count.bit_length() - 1) // 2)
    outer_count = sp_count // inner_count
    inner = lax.rem(lax.axis_index("sp"), inner_count)

    def across(shard, step):
        return lax.ppermute(shard, "sp", [(i, i ^ step) for i in range(sp_count)])

    block = width // sp_count
    half_outer = outer_count // 2

    half = sp_count // 2
    half_experts = experts // 2
    upper = lax.axis_index("sp") >= half

    def traded(shard):
        return lax.ppermute(shard, "sp", [(i, i ^ half) for i in range(sp_count)])

    facts = jnp.concatenate([route_ids.T.astype(F32), route_weights.T], axis=0)
    facts = jnp.concatenate([facts, traded(facts)], axis=1)
    stream_there = traded(stream)
    out_there = traded(out_grad)
    stream_full = in_order(stream, swapped(stream), first, 1)
    out_full = in_order(out_grad, swapped(out_grad), first, 1)
    stream_pair = jnp.concatenate(
        [stream_full, in_order(stream_there, swapped(stream_there), first, 1)], axis=0
    )
    out_pair = jnp.concatenate([out_full, in_order(out_there, swapped(out_there), first, 1)], axis=0)

    top_count = route_ids.shape[1]
    pair_ids, pair_weights = facts[:top_count].astype(jnp.int32), facts[top_count:]
    place = jnp.arange(2 * tok_rows, dtype=jnp.int32)
    block_of = place // tok_rows
    half_of = jnp.where(upper, 1 - block_of, block_of)

    def ranks(ids, expert_of, blocks, at):
        hit = ids[:, None, :] == expert_of[None, :, None]
        named = jnp.any(hit, axis=0)
        before = (at[:, None] < at[None, :]) & (blocks[:, None] == blocks[None, :])
        rank = mm(named.astype(BF), before.astype(BF), ((1,), (0,)))
        return hit, jnp.where(named, rank.astype(jnp.int32) - tp * part, -1)

    slot_at = jnp.arange(part, dtype=jnp.int32)
    here = jnp.arange(half_experts, dtype=jnp.int32) + jnp.where(upper, half_experts, 0)
    hit, slot_of = ranks(pair_ids, here, block_of, place)
    weight_of = jnp.sum(jnp.where(hit, pair_weights[:, None, :], 0.0), axis=0)
    chosen = (slot_of[:, None, None, :] == slot_at[None, None, :, None]) & (
        half_of[None, None, None, :] == jnp.arange(2, dtype=jnp.int32)[None, :, None, None]
    )
    pick = chosen.astype(BF).reshape(slots, 2 * tok_rows)
    slot_weight = jnp.sum(jnp.where(chosen, weight_of[:, None, None, :], 0.0), axis=3).reshape(slots, 1)

    half_groups = [[h * half + i for i in range(half)] for h in range(2)]
    send_rows = mm(pick, stream_pair, ((1,), (0,))).astype(BF)
    send_cot = (mm(pick, out_pair, ((1,), (0,))) * slot_weight).astype(BF)
    rows = exchanged(send_rows.reshape(half, 2 * part, width), half_groups).reshape(slots, width)
    cot = exchanged(send_cot.reshape(half, 2 * part, width), half_groups).reshape(slots, width)

    depth = taps.shape[0]
    channels = conv_gate.shape[1]
    prod_rows = conv_gate.astype(F32) * conv_value.astype(F32)
    left_rows = passed_along(prod_rows[tok_rows - depth + 1 :], "sp", 1)
    padded = jnp.concatenate([left_rows, prod_rows], axis=0)
    conv_sum = jnp.zeros((tok_rows, channels), F32)
    for tap_index in range(depth):
        conv_sum = conv_sum + taps[tap_index][None, :] * padded[tap_index : tap_index + tok_rows]
    mixer_out = (gate_in.astype(F32) * conv_sum).astype(BF)

    wide_mixer, out_cut, group_ids = [mixer_out], [], [route_ids.T.astype(F32)]
    for step in range(inner_count):
        piece = jnp.concatenate(
            [
                lax.dynamic_slice_in_dim(out_grad, (o * inner_count + (inner ^ step)) * block, block, 1)
                for o in range(half_outer)
            ],
            axis=1,
        )
        if step:
            group_ids.append(across(group_ids[0], step))
            piece = across(piece, step)
            wide_mixer.append(across(mixer_out, step))
        out_cut.append(piece)
    wide_mixer = jnp.concatenate(wide_mixer, axis=0)
    group_ids = jnp.concatenate(group_ids, axis=1).astype(jnp.int32)
    out_cut = jnp.concatenate(out_cut, axis=0)
    out_cut = in_order(out_cut, swapped(out_cut), first, 1)
    group_place = jnp.arange(inner_count * tok_rows, dtype=jnp.int32)
    group_block = group_place // tok_rows
    _, slot_group = ranks(group_ids, jnp.arange(experts, dtype=jnp.int32), group_block, group_place)
    pick_group = (slot_group[:, None, :] == slot_at[None, :, None]).astype(BF)
    pick_group = pick_group.reshape(slots, inner_count * tok_rows).T

    gate_swap, up_swap, down_swap = swapped(w_gate[0]), swapped(w_up[0]), swapped(w_down[0])
    gate_all = jnp.concatenate([w_gate[0], gate_swap], axis=1)
    up_all = jnp.concatenate([w_up[0], up_swap], axis=1)
    down_all = jnp.concatenate([w_down[0], down_swap], axis=0)
    hid = w_gate.shape[2]

    pre_gate = mm(rows, gate_all, ((1,), (0,)))
    pre_up = mm(rows, up_all, ((1,), (0,)))
    sigmoid_gate = jax.nn.sigmoid(pre_gate)
    silu_gate = pre_gate * sigmoid_gate
    hidden = (silu_gate * pre_up).astype(BF)
    slope = pre_up * sigmoid_gate * (1.0 + pre_gate * (1.0 - sigmoid_gate))
    hidden, silu_gate, slope = lax.optimization_barrier((hidden, silu_gate, slope))
    cut = width // inner_count
    gate_grad, up_grad, row_grad = row_grads(
        cot, down_all, silu_gate, slope, gate_all, up_all, outer_count, inner_count, part
    )
    back = exchanged(row_grad.reshape(sp_count, inner_count * part, cut))

    rows_both = jnp.concatenate([rows, swapped(rows)], axis=0)
    cot_both = jnp.concatenate([cot, swapped(cot)], axis=0)
    gate_both = jnp.concatenate([gate_grad[:, :hid], swapped(gate_grad[:, hid:])], axis=0)
    up_both = jnp.concatenate([up_grad[:, :hid], swapped(up_grad[:, hid:])], axis=0)
    hidden_both = jnp.concatenate([hidden[:, :hid], swapped(hidden[:, hid:])], axis=0)
    gate_w_grad = mm(rows_both, gate_both, ((0,), (0,)))
    up_w_grad = mm(rows_both, up_both, ((0,), (0,)))
    down_w_grad = mm(hidden_both, cot_both, ((0,), (0,)))

    group_tokens = inner_count * tok_rows
    core_half = half_outer * block
    (mine,) = local_kernel(
        home_kernel, [(group_tokens, cut)], inner, pick_group,
        back.reshape(experts, inner_count, part, cut),
    )
    stream_cut, own_half = local_kernel(
        add_kernel, [(group_tokens, cut), (group_tokens, core_half)], tp,
        out_cut, mine, swapped(mine),
    )
    pieces = [own_half[:tok_rows]]
    for step in range(1, inner_count):
        pieces.append(across(own_half[step * tok_rows : (step + 1) * tok_rows], step))
    if block % 128 == 0:
        (stream_half,) = local_kernel(
            lambda inner_ref, *refs: place_kernel(inner_ref, block, *refs),
            [(tok_rows, half_width)], inner, *pieces,
        )
    else:
        pieces = jnp.stack(pieces)
        ordered = [lax.dynamic_index_in_dim(pieces, inner ^ i, 0, keepdims=False) for i in range(inner_count)]
        stream_half = jnp.concatenate(
            [ordered[i][:, o * block : (o + 1) * block] for o in range(half_outer) for i in range(inner_count)],
            axis=1,
        )
    stream_whole = in_order(stream_half, swapped(stream_half), first, 1)

    mixer_grad = mm(stream_whole, w_out, ((1,), (0,))).astype(BF)
    mixer_wide = mixer_grad.astype(F32)
    gate_in_grad = (mixer_wide * conv_sum).astype(BF)
    conv_inner = mixer_wide * gate_in.astype(F32)
    right_rows = passed_along(conv_inner[: depth - 1], "sp", -1)
    padded_back = jnp.concatenate([conv_inner, right_rows], axis=0)
    prod_grad = jnp.zeros((tok_rows, channels), F32)
    for tap_index in range(depth):
        offset = depth - 1 - tap_index
        prod_grad = prod_grad + taps[tap_index][None, :] * padded_back[offset : offset + tok_rows]
    conv_gate_grad = (prod_grad * conv_value.astype(F32)).astype(BF)
    conv_value_grad = (prod_grad * conv_gate.astype(F32)).astype(BF)

    partial = mm(stream_cut, wide_mixer, ((0,), (0,))).astype(BF).reshape(outer_count, block, channels)
    outer = lax.div(lax.axis_index("sp"), inner_count)
    out_proj_grad = lax.dynamic_index_in_dim(partial, outer, 0, keepdims=False).astype(F32)
    for step in range(outer_count - 1, 0, -1):
        piece = lax.dynamic_index_in_dim(partial, outer ^ step, 0, keepdims=False)
        piece = across(piece, step * inner_count)
        out_proj_grad = out_proj_grad + piece.astype(F32)

    return (
        stream_half,
        gate_in_grad,
        conv_gate_grad,
        conv_value_grad,
        out_proj_grad,
        gate_w_grad[None],
        up_w_grad[None],
        down_w_grad[None],
    )


def solution(mesh):
    placed = (
        P("sp", "tp"),
        P("sp", "tp"),
        P("sp", "tp"),
        P("sp", "tp"),
        P("sp", "tp"),
        P(None, "tp"),
        P(None, "tp"),
        P("sp", None),
        P("sp", None),
        P("sp", None, "tp"),
        P("sp", None, "tp"),
        P("sp", "tp", None),
    )
    return jax.shard_map(
        shards,
        mesh=mesh,
        in_specs=placed,
        out_specs=(
            P("sp", "tp"),
            P("sp", "tp"),
            P("sp", "tp"),
            P("sp", "tp"),
            P("sp", "tp"),
            P("sp", None, "tp"),
            P("sp", None, "tp"),
            P("sp", "tp", None),
        ),
        check_vma=False,
    )
```

```python
import functools
import jax
import jax.numpy as jnp
from jax import lax
from jax.experimental import pallas as pl
from jax.experimental.pallas import tpu as pltpu
from jax.sharding import PartitionSpec as P

BF = jnp.bfloat16
F32 = jnp.float32


def passed_along(shard, axis, by):
    count = lax.axis_size(axis)
    pairs = [(i, i + by) for i in range(count) if 0 <= i + by < count]
    return lax.ppermute(shard, axis, pairs)


def swapped(shard):
    return lax.ppermute(shard, "tp", [(0, 1), (1, 0)])


def exchanged(blocks, groups=None):
    return lax.all_to_all(
        blocks, "sp", split_axis=0, concat_axis=0, tiled=True, axis_index_groups=groups
    )


def in_order(mine, other, first, axis):
    return jnp.where(
        first,
        jnp.concatenate([mine, other], axis=axis),
        jnp.concatenate([other, mine], axis=axis),
    )


def mm(left, right, dims):
    return lax.dot_general(left, right, (dims, ((), ())), preferred_element_type=F32)


def back_kernel(first_steps, half_outer, inner_count, part, cot, down, silu, slope, gate, up, gate_grad, up_grad, row_grad):
    step = pl.program_id(0)
    tile = silu.shape[1]

    @pl.when(step < first_steps)
    def _():
        hidden_grad = mm(cot[...], down[...], ((1,), (1,)))
        at = pl.ds(pl.multiple_of(step * tile, tile), tile)
        gate_grad[:, at] = (hidden_grad * slope[...]).astype(BF)
        up_grad[:, at] = (hidden_grad * silu[...]).astype(BF)

    @pl.when(step >= first_steps)
    def _():
        cut, units = gate.shape[0] * gate.shape[2], gate.shape[3]
        rows = mm(gate_grad[...], gate[...].reshape(cut, units), ((1,), (1,)))
        rows += mm(up_grad[...], up[...].reshape(cut, units), ((1,), (1,)))
        for h in range(2):
            for o in range(half_outer):
                picked = []
                for i in range(inner_count):
                    at = ((o * inner_count + i) * 2 + h) * part
                    picked.append(rows[at : at + part])
                row_grad[h * half_outer + o, 0] = jnp.concatenate(picked, axis=0).astype(BF)


def row_grads(cot, down, silu, slope, gate, up, outer_count, inner_count, part):
    slots, width = cot.shape
    units = down.shape[0]
    tile, cut = min(units, 512), width // inner_count
    block = cut // outer_count
    first_steps = units // tile

    def early(i):
        return jnp.minimum(i, first_steps - 1)

    def late(i):
        return jnp.maximum(i - first_steps, 0)

    by_group = (outer_count, inner_count, block, units)
    kept = pl.BlockSpec((slots, units), lambda i: (0, 0))
    cols = pl.BlockSpec((slots, tile), lambda i: (0, early(i)))
    group = pl.BlockSpec((outer_count, 1, block, units), lambda i: (0, late(i), 0, 0))
    return pl.pallas_call(
        functools.partial(back_kernel, first_steps, outer_count // 2, inner_count, part),
        grid=(first_steps + inner_count,),
        in_specs=[
            pl.BlockSpec((slots, width), lambda i: (0, 0)),
            pl.BlockSpec((tile, width), lambda i: (early(i), 0)),
            cols,
            cols,
            group,
            group,
        ],
        out_specs=[
            kept,
            kept,
            pl.BlockSpec((outer_count, 1, inner_count * part, cut), lambda i: (0, late(i), 0, 0)),
        ],
        out_shape=[
            jax.ShapeDtypeStruct((slots, units), BF),
            jax.ShapeDtypeStruct((slots, units), BF),
            jax.ShapeDtypeStruct((outer_count, inner_count, inner_count * part, cut), BF),
        ],
        compiler_params=pltpu.CompilerParams(vmem_limit_bytes=62 * 2**20),
        cost_estimate=pl.CostEstimate(
            flops=6 * slots * width * units, bytes_accessed=8 * width * units, transcendentals=0
        ),
        name="row_grads",
    )(cot, down, silu, slope, gate.reshape(by_group), up.reshape(by_group))


def home_kernel(inner, pick, back, mine):
    tok_rows = pick.shape[0] // back.shape[1]
    experts, inner_count, part, cut = back.shape
    for j in range(inner_count):
        rows = back[:, inner[0] ^ j].astype(F32).reshape(experts * part, cut).astype(BF)
        at = slice(j * tok_rows, (j + 1) * tok_rows)
        mine[at] = mm(pick[at], rows, ((1,), (0,))).astype(BF)


def add_kernel(core, out_cut, mine, other, stream_cut, own_half):
    total = out_cut[...].astype(F32) + (mine[...].astype(F32) + other[...].astype(F32))
    total = total.astype(BF)
    stream_cut[...] = total
    wide = own_half.shape[1]
    own_half[...] = jnp.where(core[0] == 0, total[:, :wide], total[:, wide:])


def place_kernel(inner, block, *refs):
    pieces, out = refs[:-1], refs[-1]
    count = len(pieces)
    for j, piece in enumerate(pieces):
        for o in range(piece.shape[1] // block):
            at = pl.multiple_of((o * count + (inner[0] ^ j)) * block, block)
            out[:, pl.ds(at, block)] = piece[:, o * block : (o + 1) * block]


def deal_kernel(core, pick, mine, other, there, there_other, dealt):
    tok_rows, wide = mine.shape
    own, far = pick[:, :tok_rows], pick[:, tok_rows:]
    for at, near_rows, far_rows in ((core[0], mine, there), (1 - core[0], other, there_other)):
        rows = mm(own, near_rows[...], ((1,), (0,))) + mm(far, far_rows[...], ((1,), (0,)))
        dealt[:, pl.ds(pl.multiple_of(at * wide, 128), wide)] = rows.astype(BF)


def local_kernel(kernel, shapes, scalar, *arrays):
    vmem = pl.BlockSpec(memory_space=pltpu.MemorySpace.VMEM)
    return pl.pallas_call(
        kernel,
        in_specs=[pl.BlockSpec(memory_space=pltpu.MemorySpace.SMEM)] + [vmem] * len(arrays),
        out_specs=[vmem] * len(shapes),
        out_shape=[jax.ShapeDtypeStruct(shape, BF) for shape in shapes],
        compiler_params=pltpu.CompilerParams(vmem_limit_bytes=24 * 2**20),
    )(scalar.astype(jnp.int32).reshape(1), *arrays)


def shards(
    stream,
    out_grad,
    gate_in,
    conv_gate,
    conv_value,
    taps,
    w_out,
    route_ids,
    route_weights,
    w_gate,
    w_up,
    w_down,
):
    tok_rows, half_width = stream.shape
    width = 2 * half_width
    sp_count = lax.axis_size("sp")
    experts = w_gate.shape[0] * sp_count
    capacity = 4 * tok_rows // experts
    part = capacity // 2
    slots = experts * part
    tp = lax.axis_index("tp")
    first = tp == 0

    inner_count = 1 << ((sp_count.bit_length() - 1) // 2)
    outer_count = sp_count // inner_count
    inner = lax.rem(lax.axis_index("sp"), inner_count)

    def across(shard, step):
        return lax.ppermute(shard, "sp", [(i, i ^ step) for i in range(sp_count)])

    block = width // sp_count
    half_outer = outer_count // 2

    half = sp_count // 2
    half_experts = experts // 2
    upper = lax.axis_index("sp") >= half

    def traded(shard):
        return lax.ppermute(shard, "sp", [(i, i ^ half) for i in range(sp_count)])

    facts = jnp.concatenate([route_ids.T.astype(F32), route_weights.T], axis=0)
    facts = jnp.concatenate([facts, traded(facts)], axis=1)
    stream_there = traded(stream)
    out_there = traded(out_grad)
    stream_other, stream_there_other = swapped(stream), swapped(stream_there)
    out_full = in_order(out_grad, swapped(out_grad), first, 1)
    out_pair = jnp.concatenate([out_full, in_order(out_there, swapped(out_there), first, 1)], axis=0)

    top_count = route_ids.shape[1]
    pair_ids, pair_weights = facts[:top_count].astype(jnp.int32), facts[top_count:]
    place = jnp.arange(2 * tok_rows, dtype=jnp.int32)
    block_of = place // tok_rows
    half_of = jnp.where(upper, 1 - block_of, block_of)

    def ranks(ids, expert_of, blocks, at):
        hit = ids[:, None, :] == expert_of[None, :, None]
        named = jnp.any(hit, axis=0)
        before = (at[:, None] < at[None, :]) & (blocks[:, None] == blocks[None, :])
        rank = mm(named.astype(BF), before.astype(BF), ((1,), (0,)))
        return hit, jnp.where(named, rank.astype(jnp.int32) - tp * part, -1)

    slot_at = jnp.arange(part, dtype=jnp.int32)
    here = jnp.arange(half_experts, dtype=jnp.int32) + jnp.where(upper, half_experts, 0)
    hit, slot_of = ranks(pair_ids, here, block_of, place)
    weight_of = jnp.sum(jnp.where(hit, pair_weights[:, None, :], 0.0), axis=0)
    chosen = (slot_of[:, None, None, :] == slot_at[None, None, :, None]) & (
        half_of[None, None, None, :] == jnp.arange(2, dtype=jnp.int32)[None, :, None, None]
    )
    pick = chosen.astype(BF).reshape(slots, 2 * tok_rows)
    slot_weight = jnp.sum(jnp.where(chosen, weight_of[:, None, None, :], 0.0), axis=3).reshape(slots, 1)

    half_groups = [[h * half + i for i in range(half)] for h in range(2)]
    (send_rows,) = local_kernel(
        deal_kernel, [(slots, width)], tp,
        pick, stream, stream_other, stream_there, stream_there_other,
    )
    send_cot = (mm(pick, out_pair, ((1,), (0,))) * slot_weight).astype(BF)
    rows = exchanged(send_rows.reshape(half, 2 * part, width), half_groups).reshape(slots, width)
    cot = exchanged(send_cot.reshape(half, 2 * part, width), half_groups).reshape(slots, width)

    depth = taps.shape[0]
    channels = conv_gate.shape[1]
    prod_rows = conv_gate.astype(F32) * conv_value.astype(F32)
    left_rows = passed_along(prod_rows[tok_rows - depth + 1 :], "sp", 1)
    padded = jnp.concatenate([left_rows, prod_rows], axis=0)
    conv_sum = jnp.zeros((tok_rows, channels), F32)
    for tap_index in range(depth):
        conv_sum = conv_sum + taps[tap_index][None, :] * padded[tap_index : tap_index + tok_rows]
    mixer_out = (gate_in.astype(F32) * conv_sum).astype(BF)

    wide_mixer, out_cut, group_ids = [mixer_out], [], [route_ids.T.astype(F32)]
    for step in range(inner_count):
        piece = jnp.concatenate(
            [
                lax.dynamic_slice_in_dim(out_grad, (o * inner_count + (inner ^ step)) * block, block, 1)
                for o in range(half_outer)
            ],
            axis=1,
        )
        if step:
            group_ids.append(across(group_ids[0], step))
            piece = across(piece, step)
            wide_mixer.append(across(mixer_out, step))
        out_cut.append(piece)
    wide_mixer = jnp.concatenate(wide_mixer, axis=0)
    group_ids = jnp.concatenate(group_ids, axis=1).astype(jnp.int32)
    out_cut = jnp.concatenate(out_cut, axis=0)
    out_cut = in_order(out_cut, swapped(out_cut), first, 1)
    group_place = jnp.arange(inner_count * tok_rows, dtype=jnp.int32)
    group_block = group_place // tok_rows
    _, slot_group = ranks(group_ids, jnp.arange(experts, dtype=jnp.int32), group_block, group_place)
    pick_group = (slot_group[:, None, :] == slot_at[None, :, None]).astype(BF)
    pick_group = pick_group.reshape(slots, inner_count * tok_rows).T

    gate_swap, up_swap, down_swap = swapped(w_gate[0]), swapped(w_up[0]), swapped(w_down[0])
    gate_all = jnp.concatenate([w_gate[0], gate_swap], axis=1)
    up_all = jnp.concatenate([w_up[0], up_swap], axis=1)
    down_all = jnp.concatenate([w_down[0], down_swap], axis=0)
    hid = w_gate.shape[2]

    pre_gate = mm(rows, gate_all, ((1,), (0,)))
    pre_up = mm(rows, up_all, ((1,), (0,)))
    sigmoid_gate = jax.nn.sigmoid(pre_gate)
    silu_gate = pre_gate * sigmoid_gate
    hidden = (silu_gate * pre_up).astype(BF)
    slope = pre_up * sigmoid_gate * (1.0 + pre_gate * (1.0 - sigmoid_gate))
    hidden, silu_gate, slope = lax.optimization_barrier((hidden, silu_gate, slope))
    cut = width // inner_count
    gate_grad, up_grad, row_grad = row_grads(
        cot, down_all, silu_gate, slope, gate_all, up_all, outer_count, inner_count, part
    )
    back = exchanged(row_grad.reshape(sp_count, inner_count * part, cut))

    rows_both = jnp.concatenate([rows, swapped(rows)], axis=0)
    cot_both = jnp.concatenate([cot, swapped(cot)], axis=0)
    gate_both = jnp.concatenate([gate_grad[:, :hid], swapped(gate_grad[:, hid:])], axis=0)
    up_both = jnp.concatenate([up_grad[:, :hid], swapped(up_grad[:, hid:])], axis=0)
    hidden_both = jnp.concatenate([hidden[:, :hid], swapped(hidden[:, hid:])], axis=0)
    gate_w_grad = mm(rows_both, gate_both, ((0,), (0,)))
    up_w_grad = mm(rows_both, up_both, ((0,), (0,)))
    down_w_grad = mm(hidden_both, cot_both, ((0,), (0,)))

    group_tokens = inner_count * tok_rows
    core_half = half_outer * block
    (mine,) = local_kernel(
        home_kernel, [(group_tokens, cut)], inner, pick_group,
        back.reshape(experts, inner_count, part, cut),
    )
    stream_cut, own_half = local_kernel(
        add_kernel, [(group_tokens, cut), (group_tokens, core_half)], tp,
        out_cut, mine, swapped(mine),
    )
    pieces = [own_half[:tok_rows]]
    for step in range(1, inner_count):
        pieces.append(across(own_half[step * tok_rows : (step + 1) * tok_rows], step))
    if block % 128 == 0:
        (stream_half,) = local_kernel(
            lambda inner_ref, *refs: place_kernel(inner_ref, block, *refs),
            [(tok_rows, half_width)], inner, *pieces,
        )
    else:
        pieces = jnp.stack(pieces)
        ordered = [lax.dynamic_index_in_dim(pieces, inner ^ i, 0, keepdims=False) for i in range(inner_count)]
        stream_half = jnp.concatenate(
            [ordered[i][:, o * block : (o + 1) * block] for o in range(half_outer) for i in range(inner_count)],
            axis=1,
        )
    half_other = swapped(stream_half)
    low, high = w_out[:half_width], w_out[half_width:]
    w_mine, w_far = jnp.where(first, low, high), jnp.where(first, high, low)

    top = min(tok_rows, 16)
    first_grad = mm(stream_half[:top], w_mine, ((1,), (0,)))
    first_grad = (first_grad + mm(half_other[:top], w_far, ((1,), (0,)))).astype(BF)
    first_inner = first_grad.astype(F32) * gate_in[:top].astype(F32)
    right_rows = passed_along(first_inner[: depth - 1], "sp", -1)
    mixer_grad = mm(stream_half, w_mine, ((1,), (0,)))
    mixer_grad = (mixer_grad + mm(half_other, w_far, ((1,), (0,)))).astype(BF)
    mixer_wide = mixer_grad.astype(F32)
    gate_in_grad = (mixer_wide * conv_sum).astype(BF)
    conv_inner = mixer_wide * gate_in.astype(F32)
    padded_back = jnp.concatenate([conv_inner, right_rows], axis=0)
    prod_grad = jnp.zeros((tok_rows, channels), F32)
    for tap_index in range(depth):
        offset = depth - 1 - tap_index
        prod_grad = prod_grad + taps[tap_index][None, :] * padded_back[offset : offset + tok_rows]
    conv_gate_grad = (prod_grad * conv_value.astype(F32)).astype(BF)
    conv_value_grad = (prod_grad * conv_gate.astype(F32)).astype(BF)

    partial = mm(stream_cut, wide_mixer, ((0,), (0,))).astype(BF).reshape(outer_count, block, channels)
    outer = lax.div(lax.axis_index("sp"), inner_count)
    out_proj_grad = lax.dynamic_index_in_dim(partial, outer, 0, keepdims=False).astype(F32)
    for step in range(outer_count - 1, 0, -1):
        piece = lax.dynamic_index_in_dim(partial, outer ^ step, 0, keepdims=False)
        piece = across(piece, step * inner_count)
        out_proj_grad = out_proj_grad + piece.astype(F32)

    return (
        stream_half,
        gate_in_grad,
        conv_gate_grad,
        conv_value_grad,
        out_proj_grad,
        gate_w_grad[None],
        up_w_grad[None],
        down_w_grad[None],
    )


def solution(mesh):
    placed = (
        P("sp", "tp"),
        P("sp", "tp"),
        P("sp", "tp"),
        P("sp", "tp"),
        P("sp", "tp"),
        P(None, "tp"),
        P(None, "tp"),
        P("sp", None),
        P("sp", None),
        P("sp", None, "tp"),
        P("sp", None, "tp"),
        P("sp", "tp", None),
    )
    return jax.shard_map(
        shards,
        mesh=mesh,
        in_specs=placed,
        out_specs=(
            P("sp", "tp"),
            P("sp", "tp"),
            P("sp", "tp"),
            P("sp", "tp"),
            P("sp", "tp"),
            P("sp", None, "tp"),
            P("sp", None, "tp"),
            P("sp", "tp", None),
        ),
        check_vma=False,
    )
```
